32 devices in a mesh: sp: 8 (over z, y), tp: 4 (over x, core).
Axes of the slice: x: 2, y: 2, z: 4, core: 2. Of those that a mesh axis runs over, the one named last changes fastest.
Arguments:
- queries: bfloat16 [4096, 2048], P('sp', 'tp'), may hold values from -6 to 6
- keys: bfloat16 [4096, 512], P('sp', 'tp'), may hold values from -6 to 6
- values: bfloat16 [4096, 512], P('sp', 'tp'), may hold values from -6 to 6
- residual: bfloat16 [4096, 2048], P(('sp', 'tp')), may hold values from -0.119628906 to 0.119628906
- out_proj: bfloat16 [2048, 2048], replicated, may hold values from -0.125 to 0.125
- query_gain: float32 [128], replicated, may hold values from 0.7 to 7
- key_gain: float32 [128], replicated, may hold values from 0.7 to 7
- norm_gain: float32 [2048], replicated, may hold values from 0.1 to 1.9
- routes: int32 [4096, 4], P(('sp', 'tp')), may hold values from 0 to 31, all different within a row; in each aligned block of 128 rows (0 to 127, 128 to 255, ...) at most 32 rows name the same one
- route_weight: float32 [4096, 4], P(('sp', 'tp')), may hold values from 0.1 to 1
- expert_gate: bfloat16 [32, 2048, 256], P(('sp', 'tp')), may hold values from -0.125 to 0.125
- expert_up: bfloat16 [32, 2048, 256], P(('sp', 'tp')), may hold values from -0.125 to 0.125
- expert_down: bfloat16 [32, 256, 2048], P(('sp', 'tp')), may hold values from -0.375 to 0.375
- shared_gate: bfloat16 [2048, 256], replicated, may hold values from -0.125 to 0.125
- shared_up: bfloat16 [2048, 256], replicated, may hold values from -0.125 to 0.125
- shared_down: bfloat16 [256, 2048], replicated, may hold values from -0.375 to 0.375
Outputs:
- layer_out: bfloat16 [4096, 2048], P(('sp', 'tp'))
The draws below stay inside these ranges and needn't reach their ends.
Inputs may be any that keep to these rules, and one draw needn't show every extreme that they name: In the rows of one device (aligned blocks of 128 tokens), no expert is named by more than 32 routes; some expert is named by exactly 32 routes of some device; the 4 experts of a token differ.
All inputs are finite; a program needn't handle non-finite values.
Results may differ from the reference program's by a relative error of at most 0.023.
The reference program's roundings to bfloat16 on the way count: a program that leaves them out, or rounds other values in their place, can miss the bound.
Values may be sent and summed in bfloat16 or wider, within the bound.
A program may use at most 128 MiB of HBM per device.

```python
import math
import jax
import jax.numpy as jnp
import numpy as np
from jax import lax

D = 2048
HEADS = 16
KV_HEADS = 4
HD = 128
EFF = 256
SFF = 256
GRID_W = 64
TOP = 4
SEQ = 4096
ROWS_DEV = 128
EXPERTS = 32
CAP = 32
N_SP = 8
N_TP = 4


def paired_draw(key):
    key_rows = jax.random.normal(jax.random.fold_in(key, 11), (SEQ, KV_HEADS * HD), jnp.float32)
    query_rows = jax.random.normal(jax.random.fold_in(key, 12), (SEQ, HEADS * HD), jnp.float32)
    return (jnp.clip(query_rows, -6.0, 6.0), jnp.clip(key_rows, -6.0, 6.0))


def draw_queries(key, part):
    return paired_draw(key)[0].astype(jnp.bfloat16)


def draw_keys(key, part):
    return paired_draw(key)[1].astype(jnp.bfloat16)


def gain_draw(key):
    return jax.random.uniform(key, (HD,), jnp.float32, 0.7, 1.3)


def draw_query_gain(key, part):
    return gain_draw(jax.random.fold_in(key, 21))


def draw_key_gain(key, part):
    return gain_draw(jax.random.fold_in(key, 22))


def block_scale(rng, shape, cuts, low, largest):
    def one(dim, blocks):
        heights = jax.random.uniform(jax.random.fold_in(jax.random.fold_in(rng, 6), dim), (blocks,), jnp.float32, low / len(cuts), largest / len(cuts))
        return jnp.repeat(jnp.exp(heights), shape[dim] // blocks).reshape((-1,) + (1,) * (len(shape) - dim - 1))

    loudness = one(*cuts[0])
    for cut in cuts[1:]:
        loudness = loudness * one(*cut)
    return loudness


def deal_out(own_key, own, number, rows, amount, top, limit, slope):
    ranking = jax.random.permutation(own_key, amount)
    heavy_load, common = portions_of(amount, rows * top, limit, slope, True), portions_of(amount, rows * top, limit, slope, False)
    places = jnp.arange(amount)

    def named(sizes, rotation):
        used = int((sizes > 0).sum())
        fixed = max(1, used // 4)
        passed = fixed + (places - fixed + rotation * (used - fixed)) % max(1, amount - fixed)
        return jnp.zeros((amount,), jnp.int32).at[ranking[jnp.where(places < fixed, places, passed)]].set(jnp.asarray(sizes, jnp.int32))

    sizes = jnp.where(number % 4 == 0, named(heavy_load, number // 4), named(common, number - number // 4 - 1))
    mixed = jax.random.permutation(jax.random.fold_in(own, 3), amount)
    source_of, taker = mixed[0:amount // 2 * 2:2], mixed[1:amount // 2 * 2:2]
    margin = jnp.minimum(sizes[source_of] - 1, limit - sizes[taker]) // 2
    margin = jnp.where((source_of == ranking[0]) | (taker == ranking[0]) | (sizes[taker] == 0), 0, jnp.maximum(margin, 0))
    passed = jax.random.randint(jax.random.fold_in(own, 4), (amount // 2,), 0, 1 << 20) % (margin + 1)
    sizes = sizes.at[source_of].add(-passed).at[taker].add(passed)
    members = jnp.searchsorted(jnp.cumsum(sizes), jnp.arange(rows * top), side="right").astype(jnp.int32)
    listing = members.reshape(top, rows).T
    listing = listing[jax.random.permutation(jax.random.fold_in(own, 1), rows)]
    rotation = jax.random.randint(jax.random.fold_in(own, 2), (rows, 1), 0, top)
    return jnp.take_along_axis(listing, (jnp.arange(top)[None, :] + rotation) % top, axis=1)


def portions_of(count, total, limit, lean, full):
    portions = [(1 << 20) // math.isqrt(standing ** lean) + 1 for standing in range(1, count + 1)]
    largest = limit if full else min(limit, max(-(-total // count), total * portions[0] // sum(portions)))
    least = 1 if total - largest >= count - 1 else 0
    given, rest = [largest] + [least] * (count - 1), total - largest - least * (count - 1)
    while rest > 0:
        movable = [i for i in range(1, count) if given[i] < largest] or [i for i in range(1, count) if given[i] < limit]
        pool, remaining = sum([portions[i] for i in movable]), rest
        for i in movable:
            extra = min(limit - given[i], max(1, remaining * portions[i] // pool), rest)
            given[i] = given[i] + extra
            rest = rest - extra
    return np.array(given)


def gaussian(key, shape, spread, reach, cuts=(), kind=jnp.bfloat16):
    loudness = block_scale(key, shape, cuts, -0.22, 0.18) if cuts else 1.0
    values = jax.random.normal(key, shape, jnp.float32) * spread * loudness
    return jnp.minimum(jnp.maximum(values, -reach), reach).astype(kind)


def setup_inputs(seed: int = 0) -> dict:
    key_of = jax.random.split(jax.random.key(seed), 17)
    queries = draw_queries(jax.random.fold_in(key_of[16], 71), 0)
    keys = draw_keys(jax.random.fold_in(key_of[16], 71), 0)
    values = gaussian(key_of[2], (SEQ, KV_HEADS * HD), 1.0, 6.0, ((0, 8), (1, 4)))
    residual = gaussian(key_of[3], (SEQ, D), 0.02, 0.119628906, ((0, 32),))
    out_proj = gaussian(key_of[4], (HEADS * HD, D), (HEADS * HD) ** -0.5, 0.125)
    query_gain = draw_query_gain(jax.random.fold_in(key_of[16], 71), 0)
    key_gain = draw_key_gain(jax.random.fold_in(key_of[16], 71), 0)
    norm_gain = jnp.clip(1.0 + 0.18 * jax.random.normal(key_of[7], (D,), jnp.float32), 0.1, 1.9)
    routes_keys = jax.random.split(jax.random.fold_in(key_of[8], 1), SEQ // ROWS_DEV)
    routes_turns = jax.random.permutation(jax.random.fold_in(key_of[8], 3), SEQ // ROWS_DEV)
    routes = jax.vmap(lambda own, number: deal_out(jax.random.fold_in(key_of[8], 2), own, number, ROWS_DEV, EXPERTS, TOP, CAP, 2))(routes_keys, routes_turns).reshape((SEQ, TOP))
    route_weight = jnp.clip(jnp.exp(math.log(1.0) - 2.3025851 * jax.random.uniform(key_of[9], (SEQ, TOP), jnp.float32) ** block_scale(key_of[9], (SEQ, TOP), ((0, 32),), -0.2, 0.2)), 0.1, 1.0)
    expert_gate = gaussian(key_of[10], (EXPERTS, D, EFF), D ** -0.5, 0.125, ((0, 32),))
    expert_up = gaussian(key_of[11], (EXPERTS, D, EFF), D ** -0.5, 0.125, ((0, 32),))
    expert_down = gaussian(key_of[12], (EXPERTS, EFF, D), EFF ** -0.5, 0.375, ((0, 32),))
    shared_gate = gaussian(key_of[13], (D, SFF), D ** -0.5, 0.125)
    shared_up = gaussian(key_of[14], (D, SFF), D ** -0.5, 0.125)
    shared_down = gaussian(key_of[15], (SFF, D), SFF ** -0.5, 0.375)
    return dict(queries=queries, keys=keys, values=values, residual=residual, out_proj=out_proj, query_gain=query_gain, key_gain=key_gain, norm_gain=norm_gain, routes=routes, route_weight=route_weight, expert_gate=expert_gate, expert_up=expert_up, expert_down=expert_down, shared_gate=shared_gate, shared_up=shared_up, shared_down=shared_down)


EPS = 1e-06
THETA = 10000.0

def rotate_pairs(block, cosine, sine):
    first, second = jnp.split(block, 2, axis=-1)
    return jnp.concatenate([first * cosine - second * sine, second * cosine + first * sine], axis=-1)

def normed_rotary(source, gain, heads, offset):
    count = source.shape[0]
    width = gain.shape[0]
    values_f = source.astype(jnp.float32).reshape(count, heads, width)
    values_f = values_f * lax.rsqrt(lax.optimization_barrier(jnp.mean(values_f * values_f, axis=-1, keepdims=True)) + EPS) * gain
    position = offset + jnp.arange(count, dtype=jnp.int32)
    grid_row = (position // GRID_W).astype(jnp.float32)
    grid_col = (position % GRID_W).astype(jnp.float32)
    quarter = width // 4
    inverse = jnp.power(THETA, -4.0 * jnp.arange(quarter, dtype=jnp.float32) / width)
    row_angle = (grid_row[:, None] * inverse[None, :])[:, None, :]
    col_angle = (grid_col[:, None] * inverse[None, :])[:, None, :]
    row_half, col_half = jnp.split(values_f, 2, axis=-1)
    turned = jnp.concatenate([rotate_pairs(row_half, jnp.cos(row_angle), jnp.sin(row_angle)), rotate_pairs(col_half, jnp.cos(col_angle), jnp.sin(col_angle))], axis=-1)
    return turned.reshape(count, heads * width).astype(jnp.bfloat16)

def reference(queries, keys, values, residual, out_proj, query_gain, key_gain, norm_gain, routes, route_weight, expert_gate, expert_up, expert_down, shared_gate, shared_up, shared_down):
    tokens = queries.shape[0]
    width = query_gain.shape[0]
    group = HEADS // KV_HEADS
    scale = 1.0 / math.sqrt(width)
    q_rot = normed_rotary(queries, query_gain, HEADS, 0)
    k_rot = normed_rotary(keys, key_gain, KV_HEADS, 0)
    key_f = k_rot.reshape(tokens, KV_HEADS, width).astype(jnp.float32).transpose(1, 0, 2)
    value_f = values.reshape(tokens, KV_HEADS, width).astype(jnp.float32).transpose(1, 0, 2)
    block = math.gcd(tokens, 512)
    q_blocks = q_rot.reshape(tokens // block, block, KV_HEADS, group, width).transpose(0, 2, 3, 1, 4)

    def attend_head(operands):
        query_part, key_part, value_part = operands
        scores = jnp.einsum('gqd,kd->gqk', query_part.astype(jnp.float32), key_part) * scale
        top = lax.optimization_barrier(jnp.max(scores, axis=-1, keepdims=True))
        weights = jnp.exp(scores - top)
        denom = lax.optimization_barrier(jnp.sum(weights, axis=-1, keepdims=True))
        rounded = weights.astype(jnp.bfloat16).astype(jnp.float32)
        summed = jnp.einsum('gqk,kd->gqd', rounded, value_part)
        return (summed / denom).astype(jnp.bfloat16)

    def attend_block(query_block):
        return lax.map(attend_head, (query_block, key_f, value_f))
    outputs = lax.map(attend_block, q_blocks)
    attn_heads = outputs.transpose(0, 3, 1, 2, 4).reshape(tokens, HEADS * width)
    projected = jnp.dot(attn_heads, out_proj, preferred_element_type=jnp.float32)
    hidden1 = (residual.astype(jnp.float32) + projected).astype(jnp.bfloat16)
    hidden_f = hidden1.astype(jnp.float32)
    normed = (hidden_f * lax.rsqrt(lax.optimization_barrier(jnp.mean(hidden_f * hidden_f, axis=-1, keepdims=True)) + EPS) * norm_gain).astype(jnp.bfloat16)
    shared_hidden = (jax.nn.silu(jnp.dot(normed, shared_gate, preferred_element_type=jnp.float32)) * jnp.dot(normed, shared_up, preferred_element_type=jnp.float32)).astype(jnp.bfloat16)
    shared_out = jnp.dot(shared_hidden, shared_down, preferred_element_type=jnp.float32)
    pairs = tokens * TOP
    flat_routes = routes.reshape(pairs)
    bound = N_SP * N_TP * CAP
    padded = jnp.concatenate([normed, jnp.zeros((1, normed.shape[1]), jnp.bfloat16)], axis=0)

    def one_expert(expert, buffer):
        picked = jnp.nonzero(flat_routes == expert, size=bound, fill_value=pairs)[0].astype(jnp.int32)
        rows = padded[picked // TOP]
        hidden_e = (jax.nn.silu(jnp.dot(rows, expert_gate[expert], preferred_element_type=jnp.float32)) * jnp.dot(rows, expert_up[expert], preferred_element_type=jnp.float32)).astype(jnp.bfloat16)
        result = jnp.dot(hidden_e, expert_down[expert], preferred_element_type=jnp.float32).astype(jnp.bfloat16)
        return buffer.at[picked].set(result)
    buffer = lax.fori_loop(0, EXPERTS, one_expert, jnp.zeros((pairs + 1, normed.shape[1]), jnp.bfloat16))
    routed = buffer[:pairs].reshape(tokens, TOP, normed.shape[1]).astype(jnp.float32)
    mixed = jnp.einsum('tk,tkd->td', route_weight, routed) + shared_out
    return (hidden_f + mixed).astype(jnp.bfloat16)
```

```python
import functools
import math

import jax
import jax.numpy as jnp
from jax import lax
from jax.experimental import pallas as pl
from jax.experimental.pallas import tpu as pltpu
from jax.sharding import PartitionSpec as P

GRID_W = 64
MESH = pl.DeviceIdType.MESH


EPS = 1e-06
THETA = 10000.0


def norm_rotate(block, gain, cosine, sine):
    mean = jnp.mean(block * block, axis=-1, keepdims=True)
    block = block * lax.rsqrt(mean + EPS) * gain
    quarter = block.shape[-1] // 4
    lane = lax.broadcasted_iota(jnp.int32, block.shape, 1)
    after = pltpu.roll(block, 3 * quarter, 1)
    before = pltpu.roll(block, quarter, 1)
    partner = jnp.where((lane // quarter) % 2 == 0, after, before)
    return (block * cosine + partner * sine).astype(jnp.bfloat16)


def plane_peer(z, d, planes):
    if planes == 4:
        return (z + 1 - 2 * (z % 2), z + 2 - 4 * (z // 2), 3 - z)[d - 1]
    return planes - 1 - z


def attention_kernel(
    n_sp, n_tp, planes, group,
    q_ref, k_ref, v_ref, cos_ref, sin_ref, qg_ref, kg_ref, out_ref,
    held, q_rot, top, total, accum, rows_out,
    send_z, send_y, recv_kv, send_o, recv_o,
):
    per = n_sp // planes
    me_sp = lax.axis_index("sp")
    me_tp = lax.axis_index("tp")
    z, y = me_sp // per, me_sp % per
    tok, width = k_ref.shape
    piece = tok // n_tp
    lanes = group * width
    held[me_sp, 0] = norm_rotate(
        k_ref[...].astype(jnp.float32), kg_ref[...], cos_ref[...], sin_ref[...]
    )
    held[me_sp, 1] = v_ref[...]
    barrier = pltpu.get_barrier_semaphore()
    for d in range(1, n_sp):
        pl.semaphore_signal(
            barrier, inc=1, device_id={"sp": lax.rem(me_sp + d, n_sp)}, device_id_type=MESH
        )
    for d in range(1, n_tp):
        pl.semaphore_signal(
            barrier, inc=1, device_id={"tp": lax.rem(me_tp + d, n_tp)}, device_id_type=MESH
        )
    pl.semaphore_wait(barrier, n_sp + n_tp - 2)

    def block_copy(block, target, sem):
        return pltpu.make_async_remote_copy(
            src_ref=held.at[block], dst_ref=held.at[block],
            send_sem=sem, recv_sem=recv_kv.at[block],
            device_id={"sp": target}, device_id_type=MESH,
        )

    def to_plane(slot, block):
        for d in range(1, per):
            block_copy(block, z * per + lax.rem(y + d, per), send_y.at[slot, d - 1]).start()

    for d in range(1, planes):
        if d == 1:
            block_copy(me_sp, plane_peer(z, d, planes) * per + y, send_z.at[d - 1]).start()
            to_plane(0, me_sp)
        else:
            block_copy(me_sp, plane_peer(z, d, planes) * per + y, send_z.at[d - 1]).start()
    for j in range(n_tp):
        rows = pl.ds(j * piece, piece)
        for h in range(group):
            q_rot[j, pl.ds(h * piece, piece), :] = norm_rotate(
                q_ref[rows, pl.ds(h * width, width)].astype(jnp.float32),
                qg_ref[...], cos_ref[rows, :], sin_ref[rows, :],
            )
    top[...] = jnp.full(top.shape, -1e30, jnp.float32)
    total[...] = jnp.zeros(total.shape, jnp.float32)
    accum[...] = jnp.zeros(accum.shape, jnp.float32)
    factor = math.log2(math.e) / math.sqrt(width)
    repeat = tok // width

    def attend(block, j):
        scores = lax.dot_general(
            q_rot[j], held[block, 0], (((1,), (1,)), ((), ())),
            preferred_element_type=jnp.float32,
        )
        old = top[j]
        new = jnp.maximum(old, jnp.max(scores, axis=1, keepdims=True))
        weights = jnp.exp2((scores - jnp.concatenate([new] * repeat, axis=1)) * factor)
        alpha = jnp.exp2((old - new) * factor)
        part = weights[:, :width]
        for r in range(1, repeat):
            part = part + weights[:, r * width:(r + 1) * width]
        summed = total[j] * alpha + part
        added = jnp.dot(
            weights.astype(jnp.bfloat16), held[block, 1], preferred_element_type=jnp.float32
        )
        return new, summed, accum[j] * alpha + added

    def out_copy(j):
        return pltpu.make_async_remote_copy(
            src_ref=rows_out.at[j],
            dst_ref=out_ref.at[:, pl.ds(pl.multiple_of(me_tp * lanes, 128), lanes)],
            send_sem=send_o.at[j], recv_sem=recv_o.at[me_tp],
            device_id={"tp": j}, device_id_type=MESH,
        )

    def step(block):
        @pl.loop(0, n_tp)
        def _(j):
            new, summed, acc = attend(block, j)
            top[j] = new
            total[j] = summed
            accum[j] = acc

    def arrive(block):
        block_copy(block, me_sp, send_z.at[0]).wait_recv()

    def others(plane, finish=False):
        for d in range(1, per):
            block = plane * per + lax.rem(y + d, per)
            arrive(block)
            step(block)

    step(me_sp)
    previous = z
    for d in range(1, planes):
        plane = plane_peer(z, d, planes)
        block = plane * per + y
        arrive(block)
        to_plane(d, block)
        others(previous)
        step(block)
        previous = plane
    others(previous)

    for d in range(n_tp):
        j = lax.rem(me_tp + 1 + d, n_tp)
        result = accum[j] / jnp.sum(total[j], axis=1, keepdims=True)
        result = result.astype(jnp.bfloat16)
        for h in range(group):
            rows_out[j, :, pl.ds(h * width, width)] = result[h * piece:(h + 1) * piece]
        if d < n_tp - 1:
            out_copy(j).start()
        else:
            for h in range(group):
                out_ref[:, pl.ds(pl.multiple_of(me_tp * lanes + h * width, 128), width)] = result[
                    h * piece:(h + 1) * piece
                ]
    for d in range(1, n_tp):
        source = lax.rem(me_tp + d, n_tp)
        pltpu.make_async_remote_copy(
            src_ref=rows_out.at[source],
            dst_ref=out_ref.at[:, pl.ds(pl.multiple_of(source * lanes, 128), lanes)],
            send_sem=send_o.at[source], recv_sem=recv_o.at[source],
            device_id={"tp": source}, device_id_type=MESH,
        ).wait()
    for d in range(1, planes):
        block_copy(me_sp, me_sp, send_z.at[d - 1]).wait_send()
    for slot in range(planes):
        for d in range(1, per):
            block_copy(me_sp, me_sp, send_y.at[slot, d - 1]).wait_send()


def attention(mesh_sp, mesh_tp, queries, keys, values, query_gain, key_gain):
    tok, width = keys.shape
    group = queries.shape[1] // width
    planes = 4 if mesh_sp % 4 == 0 else 2
    per = mesh_sp // planes
    piece = tok // mesh_tp
    quarter = width // 4
    inverse = jnp.power(THETA, -4.0 * jnp.arange(quarter, dtype=jnp.float32) / width)
    start = lax.axis_index("sp") * tok
    grid_rows = tok // GRID_W
    row_angle = (start // GRID_W + jnp.arange(grid_rows)).astype(jnp.float32)[:, None] * inverse
    col_angle = jnp.arange(GRID_W).astype(jnp.float32)[:, None] * inverse

    def spread(row_part, col_part, sign):
        row_part = jnp.broadcast_to(row_part[:, None, :], (grid_rows, GRID_W, quarter))
        col_part = jnp.broadcast_to(col_part[None, :, :], (grid_rows, GRID_W, quarter))
        return jnp.concatenate(
            [sign * row_part, row_part, sign * col_part, col_part], axis=-1
        ).reshape(tok, width)

    tables = lax.optimization_barrier(
        (jnp.cos(row_angle), jnp.cos(col_angle), jnp.sin(row_angle), jnp.sin(col_angle))
    )
    cosine = spread(tables[0], tables[1], 1.0)
    sine = spread(tables[2], tables[3], -1.0)
    vmem = pl.BlockSpec(memory_space=pltpu.VMEM)
    return pl.pallas_call(
        functools.partial(attention_kernel, mesh_sp, mesh_tp, planes, group),
        out_shape=jax.ShapeDtypeStruct((piece, mesh_tp * group * width), jnp.bfloat16),
        in_specs=[vmem] * 7,
        out_specs=vmem,
        scratch_shapes=[
            pltpu.VMEM((mesh_sp, 2, tok, width), jnp.bfloat16),
            pltpu.VMEM((mesh_tp, group * piece, width), jnp.bfloat16),
            pltpu.VMEM((mesh_tp, group * piece, width), jnp.float32),
            pltpu.VMEM((mesh_tp, group * piece, width), jnp.float32),
            pltpu.VMEM((mesh_tp, group * piece, width), jnp.float32),
            pltpu.VMEM((mesh_tp, piece, group * width), jnp.bfloat16),
            pltpu.SemaphoreType.DMA((planes - 1,)),
            pltpu.SemaphoreType.DMA((planes, max(per - 1, 1))),
            pltpu.SemaphoreType.DMA((mesh_sp,)),
            pltpu.SemaphoreType.DMA((mesh_tp,)),
            pltpu.SemaphoreType.DMA((mesh_tp,)),
        ],
        compiler_params=pltpu.CompilerParams(
            collective_id=0, has_side_effects=True, vmem_limit_bytes=48 * 2**20
        ),
        name="attention",
    )(queries, keys, values, cosine, sine, query_gain.reshape(1, width), key_gain.reshape(1, width))


def expert_apply(arrived, expert_gate, expert_up, expert_down):
    sources, slots, width = arrived.shape
    local = expert_gate.shape[0]
    grouped = arrived.reshape(sources // local, local, slots, width)
    gate_part = jnp.einsum(
        "sech,ehf->secf", grouped, expert_gate, preferred_element_type=jnp.float32
    )
    up_part = jnp.einsum("sech,ehf->secf", grouped, expert_up, preferred_element_type=jnp.float32)
    hidden_e = (jax.nn.silu(gate_part) * up_part).astype(jnp.bfloat16)
    result = jnp.einsum("secf,efh->sech", hidden_e, expert_down, preferred_element_type=jnp.float32)
    return result.astype(jnp.bfloat16).reshape(sources, slots, width)


def body(
    queries,
    keys,
    values,
    residual,
    out_proj,
    query_gain,
    key_gain,
    norm_gain,
    routes,
    route_weight,
    expert_gate,
    expert_up,
    expert_down,
    shared_gate,
    shared_up,
    shared_down,
):
    all_heads = attention(
        lax.axis_size("sp"), lax.axis_size("tp"), queries, keys, values, query_gain, key_gain
    )
    projected = jnp.dot(all_heads, out_proj, preferred_element_type=jnp.float32)
    hidden1 = (residual.astype(jnp.float32) + projected).astype(jnp.bfloat16)
    hidden_f = hidden1.astype(jnp.float32)
    normed = (
        hidden_f
        * lax.rsqrt(jnp.mean(hidden_f * hidden_f, axis=-1, keepdims=True) + EPS)
        * norm_gain
    ).astype(jnp.bfloat16)
    rows_local = normed.shape[0]
    top_count = routes.shape[1]
    pair_count = rows_local * top_count
    expert_total = expert_gate.shape[0] * lax.axis_size("sp") * lax.axis_size("tp")
    capacity = max(2, 2 * rows_local * top_count // expert_total)
    flat_routes = routes.reshape(pair_count)
    one_hot = (flat_routes[:, None] == jnp.arange(expert_total, dtype=jnp.int32)[None, :]).astype(
        jnp.float32
    )
    lower = (jnp.arange(pair_count)[:, None] >= jnp.arange(pair_count)[None, :]).astype(jnp.float32)
    running_count = jnp.dot(lower, one_hot, precision=lax.Precision.HIGHEST)
    slot_place = (jnp.sum(running_count * one_hot, axis=1) - 1.0).astype(jnp.int32)
    slot_index = flat_routes * capacity + slot_place
    slot_total = expert_total * capacity
    chosen = jnp.arange(slot_total, dtype=jnp.int32)[None, :, None] == slot_index.reshape(
        rows_local, 1, top_count
    )
    placement = jnp.any(chosen, axis=2).astype(jnp.bfloat16)
    weighted = jnp.sum(jnp.where(chosen, route_weight[:, None, :], 0.0), axis=2)
    send_rows = lax.dot_general(
        placement, normed, (((0,), (0,)), ((), ())), preferred_element_type=jnp.float32
    ).astype(jnp.bfloat16)
    send_rows = send_rows.reshape(expert_total, capacity, normed.shape[1])
    shared_hidden = (
        jax.nn.silu(jnp.dot(normed, shared_gate, preferred_element_type=jnp.float32))
        * jnp.dot(normed, shared_up, preferred_element_type=jnp.float32)
    ).astype(jnp.bfloat16)
    shared_out = jnp.dot(shared_hidden, shared_down, preferred_element_type=jnp.float32)
    processed = expert_apply(
        lax.all_to_all(send_rows, ("sp", "tp"), split_axis=0, concat_axis=0, tiled=True),
        expert_gate,
        expert_up,
        expert_down,
    )
    returned = lax.all_to_all(processed, ("sp", "tp"), split_axis=0, concat_axis=0, tiled=True)
    returned = returned.reshape(slot_total, normed.shape[1])
    mixed = shared_out + jnp.dot(
        weighted.astype(jnp.bfloat16), returned, preferred_element_type=jnp.float32
    )
    return (hidden_f + mixed).astype(jnp.bfloat16)


def solution(mesh):
    placed = (
        P("sp", "tp"),
        P("sp", "tp"),
        P("sp", "tp"),
        P(("sp", "tp"), None),
        P(),
        P(),
        P(),
        P(),
        P(("sp", "tp"), None),
        P(("sp", "tp"), None),
        P(("sp", "tp"), None, None),
        P(("sp", "tp"), None, None),
        P(("sp", "tp"), None, None),
        P(),
        P(),
        P(),
    )
    return jax.shard_map(
        body, mesh=mesh, in_specs=placed, out_specs=P(("sp", "tp"), None), check_vma=False
    )
```

```python
import functools
import math

import jax
import jax.numpy as jnp
from jax import lax
from jax.experimental import pallas as pl
from jax.experimental.pallas import tpu as pltpu
from jax.sharding import PartitionSpec as P

GRID_W = 64
MESH = pl.DeviceIdType.MESH


EPS = 1e-06
THETA = 10000.0


def norm_rotate(block, gain, cosine, sine):
    mean = jnp.mean(block * block, axis=-1, keepdims=True)
    block = block * lax.rsqrt(mean + EPS) * gain
    quarter = block.shape[-1] // 4
    lane = lax.broadcasted_iota(jnp.int32, block.shape, 1)
    after = pltpu.roll(block, 3 * quarter, 1)
    before = pltpu.roll(block, quarter, 1)
    partner = jnp.where((lane // quarter) % 2 == 0, after, before)
    return (block * cosine + partner * sine).astype(jnp.bfloat16)


def plane_peer(z, d, planes):
    if planes == 4:
        return (z + 1 - 2 * (z % 2), z + 2 - 4 * (z // 2), 3 - z)[d - 1]
    return planes - 1 - z


def attention_kernel(
    n_sp, n_tp, planes, group,
    q_ref, k_ref, v_ref, cos_ref, sin_ref, qg_ref, kg_ref, out_ref,
    held, q_rot, top, total, accum, rows_out,
    send_z, send_y, recv_kv, send_o, recv_o,
):
    per = n_sp // planes
    me_sp = lax.axis_index("sp")
    me_tp = lax.axis_index("tp")
    z, y = me_sp // per, me_sp % per
    tok, width = k_ref.shape
    piece = tok // n_tp
    lanes = group * width
    held[me_sp, 0] = norm_rotate(
        k_ref[...].astype(jnp.float32), kg_ref[...], cos_ref[...], sin_ref[...]
    )
    held[me_sp, 1] = v_ref[...]
    barrier = pltpu.get_barrier_semaphore()
    for d in range(1, n_sp):
        pl.semaphore_signal(
            barrier, inc=1, device_id={"sp": lax.rem(me_sp + d, n_sp)}, device_id_type=MESH
        )
    for d in range(1, n_tp):
        pl.semaphore_signal(
            barrier, inc=1, device_id={"tp": lax.rem(me_tp + d, n_tp)}, device_id_type=MESH
        )
    pl.semaphore_wait(barrier, n_sp + n_tp - 2)

    def block_copy(block, target, sem):
        return pltpu.make_async_remote_copy(
            src_ref=held.at[block], dst_ref=held.at[block],
            send_sem=sem, recv_sem=recv_kv.at[block],
            device_id={"sp": target}, device_id_type=MESH,
        )

    def to_plane(slot, block):
        for d in range(1, per):
            block_copy(block, z * per + lax.rem(y + d, per), send_y.at[slot, d - 1]).start()

    for d in range(1, planes):
        if d == 1:
            block_copy(me_sp, plane_peer(z, d, planes) * per + y, send_z.at[d - 1]).start()
            to_plane(0, me_sp)
        else:
            block_copy(me_sp, plane_peer(z, d, planes) * per + y, send_z.at[d - 1]).start()
    for j in range(n_tp):
        rows = pl.ds(j * piece, piece)
        for h in range(group):
            q_rot[j, pl.ds(h * piece, piece), :] = norm_rotate(
                q_ref[rows, pl.ds(h * width, width)].astype(jnp.float32),
                qg_ref[...], cos_ref[rows, :], sin_ref[rows, :],
            )
    top[...] = jnp.full(top.shape, -1e30, jnp.float32)
    total[...] = jnp.zeros(total.shape, jnp.float32)
    accum[...] = jnp.zeros(accum.shape, jnp.float32)
    factor = math.log2(math.e) / math.sqrt(width)
    repeat = tok // width

    def attend(block, j):
        scores = lax.dot_general(
            q_rot[j], held[block, 0], (((1,), (1,)), ((), ())),
            preferred_element_type=jnp.float32,
        )
        old = top[j]
        new = jnp.maximum(old, jnp.max(scores, axis=1, keepdims=True))
        weights = jnp.exp2((scores - jnp.concatenate([new] * repeat, axis=1)) * factor)
        alpha = jnp.exp2((old - new) * factor)
        part = weights[:, :width]
        for r in range(1, repeat):
            part = part + weights[:, r * width:(r + 1) * width]
        summed = total[j] * alpha + part
        added = jnp.dot(
            weights.astype(jnp.bfloat16), held[block, 1], preferred_element_type=jnp.float32
        )
        return new, summed, accum[j] * alpha + added

    def out_copy(j):
        return pltpu.make_async_remote_copy(
            src_ref=rows_out.at[j],
            dst_ref=out_ref.at[:, pl.ds(pl.multiple_of(me_tp * lanes, 128), lanes)],
            send_sem=send_o.at[j], recv_sem=recv_o.at[me_tp],
            device_id={"tp": j}, device_id_type=MESH,
        )

    def step(block):
        @pl.loop(0, n_tp)
        def _(j):
            new, summed, acc = attend(block, j)
            top[j] = new
            total[j] = summed
            accum[j] = acc

    def arrive(block):
        block_copy(block, me_sp, send_z.at[0]).wait_recv()

    def others(plane, finish=False):
        for d in range(1, per):
            block = plane * per + lax.rem(y + d, per)
            arrive(block)
            step(block)

    step(me_sp)
    previous = z
    for d in range(1, planes):
        plane = plane_peer(z, d, planes)
        block = plane * per + y
        arrive(block)
        to_plane(d, block)
        others(previous)
        step(block)
        previous = plane
    others(previous)

    for d in range(n_tp):
        j = lax.rem(me_tp + 1 + d, n_tp)
        result = accum[j] / jnp.sum(total[j], axis=1, keepdims=True)
        result = result.astype(jnp.bfloat16)
        for h in range(group):
            rows_out[j, :, pl.ds(h * width, width)] = result[h * piece:(h + 1) * piece]
        if d < n_tp - 1:
            out_copy(j).start()
        else:
            for h in range(group):
                out_ref[:, pl.ds(pl.multiple_of(me_tp * lanes + h * width, 128), width)] = result[
                    h * piece:(h + 1) * piece
                ]
    for d in range(1, n_tp):
        source = lax.rem(me_tp + d, n_tp)
        pltpu.make_async_remote_copy(
            src_ref=rows_out.at[source],
            dst_ref=out_ref.at[:, pl.ds(pl.multiple_of(source * lanes, 128), lanes)],
            send_sem=send_o.at[source], recv_sem=recv_o.at[source],
            device_id={"tp": source}, device_id_type=MESH,
        ).wait()
    for d in range(1, planes):
        block_copy(me_sp, me_sp, send_z.at[d - 1]).wait_send()
    for slot in range(planes):
        for d in range(1, per):
            block_copy(me_sp, me_sp, send_y.at[slot, d - 1]).wait_send()


def attention(mesh_sp, mesh_tp, queries, keys, values, query_gain, key_gain):
    tok, width = keys.shape
    group = queries.shape[1] // width
    planes = 4 if mesh_sp % 4 == 0 else 2
    per = mesh_sp // planes
    piece = tok // mesh_tp
    quarter = width // 4
    inverse = jnp.power(THETA, -4.0 * jnp.arange(quarter, dtype=jnp.float32) / width)
    start = lax.axis_index("sp") * tok
    grid_rows = tok // GRID_W
    row_angle = (start // GRID_W + jnp.arange(grid_rows)).astype(jnp.float32)[:, None] * inverse
    col_angle = jnp.arange(GRID_W).astype(jnp.float32)[:, None] * inverse

    def spread(row_part, col_part, sign):
        row_part = jnp.broadcast_to(row_part[:, None, :], (grid_rows, GRID_W, quarter))
        col_part = jnp.broadcast_to(col_part[None, :, :], (grid_rows, GRID_W, quarter))
        return jnp.concatenate(
            [sign * row_part, row_part, sign * col_part, col_part], axis=-1
        ).reshape(tok, width)

    tables = lax.optimization_barrier(
        (jnp.cos(row_angle), jnp.cos(col_angle), jnp.sin(row_angle), jnp.sin(col_angle))
    )
    cosine = spread(tables[0], tables[1], 1.0)
    sine = spread(tables[2], tables[3], -1.0)
    vmem = pl.BlockSpec(memory_space=pltpu.VMEM)
    return pl.pallas_call(
        functools.partial(attention_kernel, mesh_sp, mesh_tp, planes, group),
        out_shape=jax.ShapeDtypeStruct((piece, mesh_tp * group * width), jnp.bfloat16),
        in_specs=[vmem] * 7,
        out_specs=vmem,
        scratch_shapes=[
            pltpu.VMEM((mesh_sp, 2, tok, width), jnp.bfloat16),
            pltpu.VMEM((mesh_tp, group * piece, width), jnp.bfloat16),
            pltpu.VMEM((mesh_tp, group * piece, width), jnp.float32),
            pltpu.VMEM((mesh_tp, group * piece, width), jnp.float32),
            pltpu.VMEM((mesh_tp, group * piece, width), jnp.float32),
            pltpu.VMEM((mesh_tp, piece, group * width), jnp.bfloat16),
            pltpu.SemaphoreType.DMA((planes - 1,)),
            pltpu.SemaphoreType.DMA((planes, max(per - 1, 1))),
            pltpu.SemaphoreType.DMA((mesh_sp,)),
            pltpu.SemaphoreType.DMA((mesh_tp,)),
            pltpu.SemaphoreType.DMA((mesh_tp,)),
        ],
        compiler_params=pltpu.CompilerParams(
            collective_id=0, has_side_effects=True, vmem_limit_bytes=40 * 2**20
        ),
        name="attention",
    )(queries, keys, values, cosine, sine, query_gain.reshape(1, width), key_gain.reshape(1, width))


def expert_kernel(
    n_sp, n_tp, planes, cap, top_count, chunks,
    info_ref, normed_ref, hidden_ref, gate_ref, up_ref, down_ref,
    sgate_ref, sup_ref, sdown_ref, out_ref,
    info, gathered, sent, arrived, answers, returned, partial, sums,
    place, combine, acc, hid,
    s_info, r_info, s_z, r_z, s_in, r_in, s_back, r_back, s_sum, r_sum,
):
    per = n_sp // planes
    team = per * n_tp
    me_sp = lax.axis_index("sp")
    me_tp = lax.axis_index("tp")
    z, y = me_sp // per, me_sp % per
    me = y * n_tp + me_tp
    rows = normed_ref.shape[0]
    wide = normed_ref.shape[1] // chunks
    share = planes * cap
    slots = team * share
    tile = math.gcd(slots, 256)

    def in_plane(p):
        return {"sp": z * per + p // n_tp, "tp": p % n_tp}

    def at_plane(d):
        return {"sp": plane_peer(z, d, planes) * per + y}

    def block(p, size):
        return pl.ds(pl.multiple_of(p * size, size), size)

    def remote(src, dst, send, recv, target):
        return pltpu.make_async_remote_copy(
            src_ref=src, dst_ref=dst, send_sem=send, recv_sem=recv,
            device_id=target, device_id_type=MESH,
        )

    def cols(c):
        return pl.ds(c * wide, wide)

    barrier = pltpu.get_barrier_semaphore()

    @pl.loop(1, team)
    def _(d):
        pl.semaphore_signal(
            barrier, inc=1, device_id=in_plane(lax.rem(me + d, team)), device_id_type=MESH
        )

    for d in range(1, planes):
        pl.semaphore_signal(barrier, inc=1, device_id=at_plane(d), device_id_type=MESH)
    pl.semaphore_wait(barrier, team + planes - 2)

    def info_copy(d, source):
        return remote(info_ref, info.at[source], s_info.at[d], r_info.at[source], at_plane(d))

    def z_copy(c, d, source):
        return remote(
            normed_ref.at[:, cols(c)], gathered.at[c, block(source, rows)],
            s_z.at[c, d], r_z.at[c, source], at_plane(d),
        )

    def in_copy(c, p, source):
        return remote(
            sent.at[c, block(p, share)], arrived.at[c, block(source, share)],
            s_in.at[c, p], r_in.at[c, source], in_plane(p),
        )

    def back_copy(c, p, source):
        return remote(
            answers.at[c, block(p, share)], returned.at[c, block(source, share)],
            s_back.at[c, p], r_back.at[c, source], in_plane(p),
        )

    def sum_copy(c, d, source):
        return remote(
            partial.at[c, block(plane_peer(z, d, planes), rows)], sums.at[c, source],
            s_sum.at[c, d], r_sum.at[c, source], at_plane(d),
        )

    for d in range(1, planes):
        info_copy(d, z).start()
    for c in range(chunks):
        for d in range(1, planes):
            z_copy(c, d, z).start()
        gathered[c, block(z, rows)] = normed_ref[:, cols(c)]
    info[z] = info_ref[...]

    shared_gate = jnp.dot(normed_ref[...], sgate_ref[...], preferred_element_type=jnp.float32)
    shared_up = jnp.dot(normed_ref[...], sup_ref[...], preferred_element_type=jnp.float32)
    shared_hid = (jax.nn.silu(shared_gate) * shared_up).astype(jnp.bfloat16)
    for c in range(chunks):
        out_ref[:, cols(c)] = jnp.dot(
            shared_hid, sdown_ref[:, cols(c)], preferred_element_type=jnp.float32
        ) + hidden_ref[:, cols(c)].astype(jnp.float32)

    number = lax.broadcasted_iota(jnp.int32, (slots, rows), 0)
    owner = (number // cap) % planes
    slot = ((z * team + number // share) * cap + number % cap).astype(jnp.float32)
    for d in range(1, planes):
        info_copy(d, plane_peer(z, d, planes)).wait_recv()
    for plane in range(planes):
        wanted = jnp.where(owner == plane, slot, -1.0)
        ones = jnp.zeros((slots, rows), jnp.float32)
        shares = jnp.zeros((slots, rows), jnp.float32)
        for k in range(top_count):
            match = wanted == info[plane, k:k + 1, :]
            ones = jnp.where(match, 1.0, ones)
            shares = jnp.where(match, info[plane, top_count + k:top_count + k + 1, :], shares)
        place[:, pl.ds(plane * rows, rows)] = ones.astype(jnp.bfloat16)
        combine[pl.ds(plane * rows, rows), :] = shares.T.astype(jnp.bfloat16)

    for c in range(chunks):
        for d in range(1, planes):
            z_copy(c, d, plane_peer(z, d, planes)).wait_recv()

        @pl.loop(0, slots // tile)
        def _(i):
            sent[c, block(i, tile)] = jnp.dot(
                place[block(i, tile), :], gathered[c], preferred_element_type=jnp.float32
            ).astype(jnp.bfloat16)

        @pl.loop(1, team)
        def _(d):
            in_copy(c, lax.rem(me + d, team), me).start()

        arrived[c, block(me, share)] = sent[c, block(me, share)]

    inner = gate_ref.shape[2]
    for c in range(chunks):
        @pl.loop(1, team)
        def _(d):
            source = lax.rem(me + d, team)
            in_copy(c, source, source).wait_recv()

        @pl.loop(0, slots // tile)
        def _(i):
            part = arrived[c, block(i, tile)]
            gate = jnp.dot(part, gate_ref[0, cols(c), :], preferred_element_type=jnp.float32)
            up = jnp.dot(part, up_ref[0, cols(c), :], preferred_element_type=jnp.float32)
            if c > 0:
                gate = gate + acc[block(i, tile), pl.ds(0, inner)]
                up = up + acc[block(i, tile), pl.ds(inner, inner)]
            if c < chunks - 1:
                acc[block(i, tile), pl.ds(0, inner)] = gate
                acc[block(i, tile), pl.ds(inner, inner)] = up
            else:
                hid[block(i, tile), :] = (jax.nn.silu(gate) * up).astype(jnp.bfloat16)

    for c in range(chunks):
        @pl.loop(0, slots // tile)
        def _(i):
            answers[c, block(i, tile)] = jnp.dot(
                hid[block(i, tile), :], down_ref[0, :, cols(c)],
                preferred_element_type=jnp.float32,
            ).astype(jnp.bfloat16)

        @pl.loop(1, team)
        def _(d):
            back_copy(c, lax.rem(me + d, team), me).start()

        returned[c, block(me, share)] = answers[c, block(me, share)]

    for c in range(chunks):
        @pl.loop(1, team)
        def _(d):
            source = lax.rem(me + d, team)
            back_copy(c, source, source).wait_recv()

        @pl.loop(0, planes)
        def _(i):
            partial[c, block(i, rows)] = jnp.dot(
                combine[block(i, rows), :], returned[c], preferred_element_type=jnp.float32
            ).astype(jnp.bfloat16)

        for d in range(1, planes):
            sum_copy(c, d, z).start()
        sums[c, z] = partial[c, block(z, rows)]

    for c in range(chunks):
        for d in range(1, planes):
            sum_copy(c, d, plane_peer(z, d, planes)).wait_recv()
        result = out_ref[:, cols(c)]
        for plane in range(planes):
            result = result + sums[c, plane].astype(jnp.float32)
        out_ref[:, cols(c)] = result

    for d in range(1, planes):
        info_copy(d, z).wait_send()
    for c in range(chunks):
        for d in range(1, planes):
            z_copy(c, d, z).wait_send()
            sum_copy(c, d, z).wait_send()

        @pl.loop(1, team)
        def _(d):
            p = lax.rem(me + d, team)
            in_copy(c, p, me).wait_send()
            back_copy(c, p, me).wait_send()


def routed_experts(
    info, normed, hidden1, gate, up, down, shared_gate, shared_up, shared_down, cap
):
    n_sp, n_tp = lax.axis_size("sp"), lax.axis_size("tp")
    rows, model = normed.shape
    planes = 4 if n_sp % 4 == 0 else 2
    team = n_sp // planes * n_tp
    chunks = 4
    wide = model // chunks
    slots = team * planes * cap
    inner = gate.shape[2]
    top_count = info.shape[0] // 2
    vmem = pl.BlockSpec(memory_space=pltpu.VMEM)
    dma = pltpu.SemaphoreType.DMA
    return pl.pallas_call(
        functools.partial(expert_kernel, n_sp, n_tp, planes, cap, top_count, chunks),
        out_shape=jax.ShapeDtypeStruct((rows, model), jnp.float32),
        in_specs=[vmem] * 9,
        out_specs=vmem,
        scratch_shapes=[
            pltpu.VMEM((planes,) + info.shape, jnp.float32),
            pltpu.VMEM((chunks, planes * rows, wide), jnp.bfloat16),
            pltpu.VMEM((chunks, slots, wide), jnp.bfloat16),
            pltpu.VMEM((chunks, slots, wide), jnp.bfloat16),
            pltpu.VMEM((chunks, slots, wide), jnp.bfloat16),
            pltpu.VMEM((chunks, slots, wide), jnp.bfloat16),
            pltpu.VMEM((chunks, planes * rows, wide), jnp.bfloat16),
            pltpu.VMEM((chunks, planes, rows, wide), jnp.bfloat16),
            pltpu.VMEM((slots, planes * rows), jnp.bfloat16),
            pltpu.VMEM((planes * rows, slots), jnp.bfloat16),
            pltpu.VMEM((slots, 2 * inner), jnp.float32),
            pltpu.VMEM((slots, inner), jnp.bfloat16),
            dma((planes,)), dma((planes,)),
            dma((chunks, planes)), dma((chunks, planes)),
            dma((chunks, team)), dma((chunks, team)),
            dma((chunks, team)), dma((chunks, team)),
            dma((chunks, planes)), dma((chunks, planes)),
        ],
        compiler_params=pltpu.CompilerParams(
            collective_id=1, has_side_effects=True, vmem_limit_bytes=56 * 2**20
        ),
        name="experts",
    )(info, normed, hidden1, gate, up, down, shared_gate, shared_up, shared_down)


def body(
    queries,
    keys,
    values,
    residual,
    out_proj,
    query_gain,
    key_gain,
    norm_gain,
    routes,
    route_weight,
    expert_gate,
    expert_up,
    expert_down,
    shared_gate,
    shared_up,
    shared_down,
):
    all_heads = attention(
        lax.axis_size("sp"), lax.axis_size("tp"), queries, keys, values, query_gain, key_gain
    )
    projected = jnp.dot(all_heads, out_proj, preferred_element_type=jnp.float32)
    hidden1 = (residual.astype(jnp.float32) + projected).astype(jnp.bfloat16)
    hidden_f = hidden1.astype(jnp.float32)
    normed = (
        hidden_f
        * lax.rsqrt(jnp.mean(hidden_f * hidden_f, axis=-1, keepdims=True) + EPS)
        * norm_gain
    ).astype(jnp.bfloat16)
    rows_local = normed.shape[0]
    top_count = routes.shape[1]
    pair_count = rows_local * top_count
    expert_total = expert_gate.shape[0] * lax.axis_size("sp") * lax.axis_size("tp")
    capacity = max(2, 2 * rows_local * top_count // expert_total)
    flat_routes = routes.reshape(pair_count)
    one_hot = (flat_routes[:, None] == jnp.arange(expert_total, dtype=jnp.int32)[None, :]).astype(
        jnp.float32
    )
    lower = (jnp.arange(pair_count)[:, None] >= jnp.arange(pair_count)[None, :]).astype(jnp.float32)
    running_count = jnp.dot(lower, one_hot, precision=lax.Precision.HIGHEST)
    slot_place = (jnp.sum(running_count * one_hot, axis=1) - 1.0).astype(jnp.int32)
    slot_index = flat_routes * capacity + slot_place
    slots = slot_index.reshape(rows_local, top_count).astype(jnp.float32)
    info = jnp.concatenate([slots.T, route_weight.T], axis=0)
    layer_out = routed_experts(
        info, normed, hidden1, expert_gate, expert_up, expert_down,
        shared_gate, shared_up, shared_down, capacity,
    )
    return layer_out.astype(jnp.bfloat16)


def solution(mesh):
    placed = (
        P("sp", "tp"),
        P("sp", "tp"),
        P("sp", "tp"),
        P(("sp", "tp"), None),
        P(),
        P(),
        P(),
        P(),
        P(("sp", "tp"), None),
        P(("sp", "tp"), None),
        P(("sp", "tp"), None, None),
        P(("sp", "tp"), None, None),
        P(("sp", "tp"), None, None),
        P(),
        P(),
        P(),
    )
    return jax.shard_map(
        body, mesh=mesh, in_specs=placed, out_specs=P(("sp", "tp"), None), check_vma=False
    )
```

```python
import functools
import math

import jax
import jax.numpy as jnp
from jax import lax
from jax.experimental import pallas as pl
from jax.experimental.pallas import tpu as pltpu
from jax.sharding import PartitionSpec as P

GRID_W = 64
MESH = pl.DeviceIdType.MESH


EPS = 1e-06
THETA = 10000.0


def norm_rotate(block, gain, cosine, sine):
    mean = jnp.mean(block * block, axis=-1, keepdims=True)
    block = block * lax.rsqrt(mean + EPS) * gain
    quarter = block.shape[-1] // 4
    lane = lax.broadcasted_iota(jnp.int32, block.shape, 1)
    after = pltpu.roll(block, 3 * quarter, 1)
    before = pltpu.roll(block, quarter, 1)
    partner = jnp.where((lane // quarter) % 2 == 0, after, before)
    return (block * cosine + partner * sine).astype(jnp.bfloat16)


def plane_peer(z, d, planes):
    if planes == 4:
        return (z + 1 - 2 * (z % 2), z + 2 - 4 * (z // 2), 3 - z)[d - 1]
    return planes - 1 - z


def attention_kernel(
    n_sp, n_tp, planes, group,
    q_ref, k_ref, v_ref, cos_ref, sin_ref, qg_ref, kg_ref, out_ref,
    held, q_rot, top, total, accum, rows_out,
    send_z, send_y, recv_kv, send_o, recv_o,
):
    per = n_sp // planes
    me_sp = lax.axis_index("sp")
    me_tp = lax.axis_index("tp")
    z, y = me_sp // per, me_sp % per
    tok, width = k_ref.shape
    piece = tok // n_tp
    lanes = group * width
    held[me_sp, 0] = norm_rotate(
        k_ref[...].astype(jnp.float32), kg_ref[...], cos_ref[...], sin_ref[...]
    )
    held[me_sp, 1] = v_ref[...]
    barrier = pltpu.get_barrier_semaphore()
    for d in range(1, n_sp):
        pl.semaphore_signal(
            barrier, inc=1, device_id={"sp": lax.rem(me_sp + d, n_sp)}, device_id_type=MESH
        )
    for d in range(1, n_tp):
        pl.semaphore_signal(
            barrier, inc=1, device_id={"tp": lax.rem(me_tp + d, n_tp)}, device_id_type=MESH
        )
    pl.semaphore_wait(barrier, n_sp + n_tp - 2)

    def block_copy(block, target, sem):
        return pltpu.make_async_remote_copy(
            src_ref=held.at[block], dst_ref=held.at[block],
            send_sem=sem, recv_sem=recv_kv.at[block],
            device_id={"sp": target}, device_id_type=MESH,
        )

    def to_plane(slot, block):
        for d in range(1, per):
            block_copy(block, z * per + lax.rem(y + d, per), send_y.at[slot, d - 1]).start()

    for d in range(1, planes):
        if d == 1:
            block_copy(me_sp, plane_peer(z, d, planes) * per + y, send_z.at[d - 1]).start()
            to_plane(0, me_sp)
        else:
            block_copy(me_sp, plane_peer(z, d, planes) * per + y, send_z.at[d - 1]).start()
    for j in range(n_tp):
        rows = pl.ds(j * piece, piece)
        for h in range(group):
            q_rot[j, pl.ds(h * piece, piece), :] = norm_rotate(
                q_ref[rows, pl.ds(h * width, width)].astype(jnp.float32),
                qg_ref[...], cos_ref[rows, :], sin_ref[rows, :],
            )
    top[...] = jnp.full(top.shape, -1e30, jnp.float32)
    total[...] = jnp.zeros(total.shape, jnp.float32)
    accum[...] = jnp.zeros(accum.shape, jnp.float32)
    factor = math.log2(math.e) / math.sqrt(width)
    repeat = tok // width

    def attend(block, j):
        scores = lax.dot_general(
            q_rot[j], held[block, 0], (((1,), (1,)), ((), ())),
            preferred_element_type=jnp.float32,
        )
        old = top[j]
        new = jnp.maximum(old, jnp.max(scores, axis=1, keepdims=True))
        weights = jnp.exp2((scores - jnp.concatenate([new] * repeat, axis=1)) * factor)
        alpha = jnp.exp2((old - new) * factor)
        part = weights[:, :width]
        for r in range(1, repeat):
            part = part + weights[:, r * width:(r + 1) * width]
        summed = total[j] * alpha + part
        added = jnp.dot(
            weights.astype(jnp.bfloat16), held[block, 1], preferred_element_type=jnp.float32
        )
        return new, summed, accum[j] * alpha + added

    def out_copy(j):
        return pltpu.make_async_remote_copy(
            src_ref=rows_out.at[j],
            dst_ref=out_ref.at[:, pl.ds(pl.multiple_of(me_tp * lanes, 128), lanes)],
            send_sem=send_o.at[j], recv_sem=recv_o.at[me_tp],
            device_id={"tp": j}, device_id_type=MESH,
        )

    def step(block):
        @pl.loop(0, n_tp)
        def _(j):
            new, summed, acc = attend(block, j)
            top[j] = new
            total[j] = summed
            accum[j] = acc

    def arrive(block):
        block_copy(block, me_sp, send_z.at[0]).wait_recv()

    def others(plane, finish=False):
        for d in range(1, per):
            block = plane * per + lax.rem(y + d, per)
            arrive(block)
            step(block)

    step(me_sp)
    previous = z
    for d in range(1, planes):
        plane = plane_peer(z, d, planes)
        block = plane * per + y
        arrive(block)
        to_plane(d, block)
        others(previous)
        step(block)
        previous = plane
    others(previous)

    for d in range(n_tp):
        j = lax.rem(me_tp + 1 + d, n_tp)
        result = accum[j] / jnp.sum(total[j], axis=1, keepdims=True)
        result = result.astype(jnp.bfloat16)
        for h in range(group):
            rows_out[j, :, pl.ds(h * width, width)] = result[h * piece:(h + 1) * piece]
        if d < n_tp - 1:
            out_copy(j).start()
        else:
            for h in range(group):
                out_ref[:, pl.ds(pl.multiple_of(me_tp * lanes + h * width, 128), width)] = result[
                    h * piece:(h + 1) * piece
                ]
    for d in range(1, n_tp):
        source = lax.rem(me_tp + d, n_tp)
        pltpu.make_async_remote_copy(
            src_ref=rows_out.at[source],
            dst_ref=out_ref.at[:, pl.ds(pl.multiple_of(source * lanes, 128), lanes)],
            send_sem=send_o.at[source], recv_sem=recv_o.at[source],
            device_id={"tp": source}, device_id_type=MESH,
        ).wait()
    for d in range(1, planes):
        block_copy(me_sp, me_sp, send_z.at[d - 1]).wait_send()
    for slot in range(planes):
        for d in range(1, per):
            block_copy(me_sp, me_sp, send_y.at[slot, d - 1]).wait_send()


def attention(mesh_sp, mesh_tp, queries, keys, values, query_gain, key_gain):
    tok, width = keys.shape
    group = queries.shape[1] // width
    planes = 4 if mesh_sp % 4 == 0 else 2
    per = mesh_sp // planes
    piece = tok // mesh_tp
    quarter = width // 4
    inverse = jnp.power(THETA, -4.0 * jnp.arange(quarter, dtype=jnp.float32) / width)
    start = lax.axis_index("sp") * tok
    grid_rows = tok // GRID_W
    row_angle = (start // GRID_W + jnp.arange(grid_rows)).astype(jnp.float32)[:, None] * inverse
    col_angle = jnp.arange(GRID_W).astype(jnp.float32)[:, None] * inverse

    def spread(row_part, col_part, sign):
        row_part = jnp.broadcast_to(row_part[:, None, :], (grid_rows, GRID_W, quarter))
        col_part = jnp.broadcast_to(col_part[None, :, :], (grid_rows, GRID_W, quarter))
        return jnp.concatenate(
            [sign * row_part, row_part, sign * col_part, col_part], axis=-1
        ).reshape(tok, width)

    tables = lax.optimization_barrier(
        (jnp.cos(row_angle), jnp.cos(col_angle), jnp.sin(row_angle), jnp.sin(col_angle))
    )
    cosine = spread(tables[0], tables[1], 1.0)
    sine = spread(tables[2], tables[3], -1.0)
    vmem = pl.BlockSpec(memory_space=pltpu.VMEM)
    return pl.pallas_call(
        functools.partial(attention_kernel, mesh_sp, mesh_tp, planes, group),
        out_shape=jax.ShapeDtypeStruct((piece, mesh_tp * group * width), jnp.bfloat16),
        in_specs=[vmem] * 7,
        out_specs=vmem,
        scratch_shapes=[
            pltpu.VMEM((mesh_sp, 2, tok, width), jnp.bfloat16),
            pltpu.VMEM((mesh_tp, group * piece, width), jnp.bfloat16),
            pltpu.VMEM((mesh_tp, group * piece, width), jnp.float32),
            pltpu.VMEM((mesh_tp, group * piece, width), jnp.float32),
            pltpu.VMEM((mesh_tp, group * piece, width), jnp.float32),
            pltpu.VMEM((mesh_tp, piece, group * width), jnp.bfloat16),
            pltpu.SemaphoreType.DMA((planes - 1,)),
            pltpu.SemaphoreType.DMA((planes, max(per - 1, 1))),
            pltpu.SemaphoreType.DMA((mesh_sp,)),
            pltpu.SemaphoreType.DMA((mesh_tp,)),
            pltpu.SemaphoreType.DMA((mesh_tp,)),
        ],
        compiler_params=pltpu.CompilerParams(
            collective_id=0, has_side_effects=True, vmem_limit_bytes=40 * 2**20
        ),
        name="attention",
    )(queries, keys, values, cosine, sine, query_gain.reshape(1, width), key_gain.reshape(1, width))


def expert_kernel(
    n_sp, n_tp, planes, cap, top_count, chunks,
    info_ref, normed_ref, hidden_ref, gate_ref, up_ref, down_ref,
    sgate_ref, sup_ref, sdown_ref, out_ref,
    info, gathered, sent, arrived, answers, returned, partial, sums,
    place, combine, acc, hid,
    s_info, r_info, s_z, r_z, s_in, r_in, s_back, r_back, s_sum, r_sum,
):
    per = n_sp // planes
    team = per * n_tp
    me_sp = lax.axis_index("sp")
    me_tp = lax.axis_index("tp")
    z, y = me_sp // per, me_sp % per
    me = y * n_tp + me_tp
    rows = normed_ref.shape[0]
    wide = normed_ref.shape[1] // chunks
    share = planes * cap
    slots = team * share
    tile = math.gcd(slots, 256)

    def in_plane(p):
        return {"sp": z * per + p // n_tp, "tp": p % n_tp}

    def at_plane(d):
        return {"sp": plane_peer(z, d, planes) * per + y}

    def block(p, size):
        return pl.ds(pl.multiple_of(p * size, size), size)

    def remote(src, dst, send, recv, target):
        return pltpu.make_async_remote_copy(
            src_ref=src, dst_ref=dst, send_sem=send, recv_sem=recv,
            device_id=target, device_id_type=MESH,
        )

    def cols(c):
        return pl.ds(c * wide, wide)

    barrier = pltpu.get_barrier_semaphore()

    @pl.loop(1, team)
    def _(d):
        pl.semaphore_signal(
            barrier, inc=1, device_id=in_plane(lax.rem(me + d, team)), device_id_type=MESH
        )

    for d in range(1, planes):
        pl.semaphore_signal(barrier, inc=1, device_id=at_plane(d), device_id_type=MESH)
    pl.semaphore_wait(barrier, team + planes - 2)

    def info_copy(d, source):
        return remote(info_ref, info.at[source], s_info.at[d], r_info.at[source], at_plane(d))

    def z_copy(c, d, source):
        return remote(
            normed_ref.at[:, cols(c)], gathered.at[c, block(source, rows)],
            s_z.at[c, d], r_z.at[c, source], at_plane(d),
        )

    def in_copy(c, p, source):
        return remote(
            sent.at[c, block(p, share)], arrived.at[c, block(source, share)],
            s_in.at[c, p], r_in.at[c, source], in_plane(p),
        )

    def back_copy(c, p, source):
        return remote(
            answers.at[c, block(p, share)], returned.at[c, block(source, share)],
            s_back.at[c, p], r_back.at[c, source], in_plane(p),
        )

    def sum_copy(c, d, source):
        return remote(
            partial.at[c, block(plane_peer(z, d, planes), rows)], sums.at[c, source],
            s_sum.at[c, d], r_sum.at[c, source], at_plane(d),
        )

    for d in range(1, planes):
        info_copy(d, z).start()
    for c in range(chunks):
        for d in range(1, planes):
            z_copy(c, d, z).start()
        gathered[c, block(z, rows)] = normed_ref[:, cols(c)]
    info[z] = info_ref[...]

    shared_gate = jnp.dot(normed_ref[...], sgate_ref[...], preferred_element_type=jnp.float32)
    shared_up = jnp.dot(normed_ref[...], sup_ref[...], preferred_element_type=jnp.float32)
    shared_hid = (jax.nn.silu(shared_gate) * shared_up).astype(jnp.bfloat16)
    for c in range(chunks):
        out_ref[:, cols(c)] = jnp.dot(
            shared_hid, sdown_ref[:, cols(c)], preferred_element_type=jnp.float32
        ) + hidden_ref[:, cols(c)].astype(jnp.float32)

    number = lax.broadcasted_iota(jnp.int32, (slots, rows), 0)
    owner = (number // cap) % planes
    slot = ((z * team + number // share) * cap + number % cap).astype(jnp.float32)
    for d in range(1, planes):
        info_copy(d, plane_peer(z, d, planes)).wait_recv()
    for plane in range(planes):
        wanted = jnp.where(owner == plane, slot, -1.0)
        ones = jnp.zeros((slots, rows), jnp.float32)
        shares = jnp.zeros((slots, rows), jnp.float32)
        for k in range(top_count):
            match = wanted == info[plane, k:k + 1, :]
            ones = jnp.where(match, 1.0, ones)
            shares = jnp.where(match, info[plane, top_count + k:top_count + k + 1, :], shares)
        place[:, pl.ds(plane * rows, rows)] = ones.astype(jnp.bfloat16)
        combine[pl.ds(plane * rows, rows), :] = shares.T.astype(jnp.bfloat16)

    for c in range(chunks):
        for d in range(1, planes):
            z_copy(c, d, plane_peer(z, d, planes)).wait_recv()

        @pl.loop(0, slots // tile)
        def _(i):
            sent[c, block(i, tile)] = jnp.dot(
                place[block(i, tile), :], gathered[c], preferred_element_type=jnp.float32
            ).astype(jnp.bfloat16)

        @pl.loop(1, team)
        def _(d):
            in_copy(c, lax.rem(me + d, team), me).start()

        arrived[c, block(me, share)] = sent[c, block(me, share)]

    inner = gate_ref.shape[2]
    for c in range(chunks):
        @pl.loop(1, team)
        def _(d):
            source = lax.rem(me + d, team)
            in_copy(c, source, source).wait_recv()

        @pl.loop(0, slots // tile)
        def _(i):
            part = arrived[c, block(i, tile)]
            gate = jnp.dot(part, gate_ref[0, cols(c), :], preferred_element_type=jnp.float32)
            up = jnp.dot(part, up_ref[0, cols(c), :], preferred_element_type=jnp.float32)
            if c > 0:
                gate = gate + acc[block(i, tile), pl.ds(0, inner)]
                up = up + acc[block(i, tile), pl.ds(inner, inner)]
            if c < chunks - 1:
                acc[block(i, tile), pl.ds(0, inner)] = gate
                acc[block(i, tile), pl.ds(inner, inner)] = up
            else:
                hid[block(i, tile), :] = (jax.nn.silu(gate) * up).astype(jnp.bfloat16)

    for c in range(chunks):
        @pl.loop(0, slots // tile)
        def _(i):
            answers[c, block(i, tile)] = jnp.dot(
                hid[block(i, tile), :], down_ref[0, :, cols(c)],
                preferred_element_type=jnp.float32,
            ).astype(jnp.bfloat16)

        @pl.loop(1, team)
        def _(d):
            back_copy(c, lax.rem(me + d, team), me).start()

        returned[c, block(me, share)] = answers[c, block(me, share)]

    for c in range(chunks):
        @pl.loop(1, team)
        def _(d):
            source = lax.rem(me + d, team)
            back_copy(c, source, source).wait_recv()

        @pl.loop(0, planes)
        def _(i):
            partial[c, block(i, rows)] = jnp.dot(
                combine[block(i, rows), :], returned[c], preferred_element_type=jnp.float32
            ).astype(jnp.bfloat16)

        for d in range(1, planes):
            sum_copy(c, d, z).start()
        sums[c, z] = partial[c, block(z, rows)]

    for c in range(chunks):
        for d in range(1, planes):
            sum_copy(c, d, plane_peer(z, d, planes)).wait_recv()
        result = out_ref[:, cols(c)]
        for plane in range(planes):
            result = result + sums[c, plane].astype(jnp.float32)
        out_ref[:, cols(c)] = result

    for d in range(1, planes):
        info_copy(d, z).wait_send()
    for c in range(chunks):
        for d in range(1, planes):
            z_copy(c, d, z).wait_send()
            sum_copy(c, d, z).wait_send()

        @pl.loop(1, team)
        def _(d):
            p = lax.rem(me + d, team)
            in_copy(c, p, me).wait_send()
            back_copy(c, p, me).wait_send()


def routed_experts(
    info, normed, hidden1, gate, up, down, shared_gate, shared_up, shared_down, cap
):
    n_sp, n_tp = lax.axis_size("sp"), lax.axis_size("tp")
    rows, model = normed.shape
    planes = 4 if n_sp % 4 == 0 else 2
    team = n_sp // planes * n_tp
    chunks = 8
    wide = model // chunks
    slots = team * planes * cap
    inner = gate.shape[2]
    top_count = info.shape[0] // 2
    vmem = pl.BlockSpec(memory_space=pltpu.VMEM)
    dma = pltpu.SemaphoreType.DMA
    return pl.pallas_call(
        functools.partial(expert_kernel, n_sp, n_tp, planes, cap, top_count, chunks),
        out_shape=jax.ShapeDtypeStruct((rows, model), jnp.float32),
        in_specs=[vmem] * 9,
        out_specs=vmem,
        scratch_shapes=[
            pltpu.VMEM((planes,) + info.shape, jnp.float32),
            pltpu.VMEM((chunks, planes * rows, wide), jnp.bfloat16),
            pltpu.VMEM((chunks, slots, wide), jnp.bfloat16),
            pltpu.VMEM((chunks, slots, wide), jnp.bfloat16),
            pltpu.VMEM((chunks, slots, wide), jnp.bfloat16),
            pltpu.VMEM((chunks, slots, wide), jnp.bfloat16),
            pltpu.VMEM((chunks, planes * rows, wide), jnp.bfloat16),
            pltpu.VMEM((chunks, planes, rows, wide), jnp.bfloat16),
            pltpu.VMEM((slots, planes * rows), jnp.bfloat16),
            pltpu.VMEM((planes * rows, slots), jnp.bfloat16),
            pltpu.VMEM((slots, 2 * inner), jnp.float32),
            pltpu.VMEM((slots, inner), jnp.bfloat16),
            dma((planes,)), dma((planes,)),
            dma((chunks, planes)), dma((chunks, planes)),
            dma((chunks, team)), dma((chunks, team)),
            dma((chunks, team)), dma((chunks, team)),
            dma((chunks, planes)), dma((chunks, planes)),
        ],
        compiler_params=pltpu.CompilerParams(
            collective_id=1, has_side_effects=True, vmem_limit_bytes=56 * 2**20
        ),
        name="experts",
    )(info, normed, hidden1, gate, up, down, shared_gate, shared_up, shared_down)


def body(
    queries,
    keys,
    values,
    residual,
    out_proj,
    query_gain,
    key_gain,
    norm_gain,
    routes,
    route_weight,
    expert_gate,
    expert_up,
    expert_down,
    shared_gate,
    shared_up,
    shared_down,
):
    all_heads = attention(
        lax.axis_size("sp"), lax.axis_size("tp"), queries, keys, values, query_gain, key_gain
    )
    projected = jnp.dot(all_heads, out_proj, preferred_element_type=jnp.float32)
    hidden1 = (residual.astype(jnp.float32) + projected).astype(jnp.bfloat16)
    hidden_f = hidden1.astype(jnp.float32)
    normed = (
        hidden_f
        * lax.rsqrt(jnp.mean(hidden_f * hidden_f, axis=-1, keepdims=True) + EPS)
        * norm_gain
    ).astype(jnp.bfloat16)
    rows_local = normed.shape[0]
    top_count = routes.shape[1]
    pair_count = rows_local * top_count
    expert_total = expert_gate.shape[0] * lax.axis_size("sp") * lax.axis_size("tp")
    capacity = max(2, 2 * rows_local * top_count // expert_total)
    flat_routes = routes.reshape(pair_count)
    one_hot = (flat_routes[:, None] == jnp.arange(expert_total, dtype=jnp.int32)[None, :]).astype(
        jnp.float32
    )
    lower = (jnp.arange(pair_count)[:, None] >= jnp.arange(pair_count)[None, :]).astype(jnp.float32)
    running_count = jnp.dot(lower, one_hot, precision=lax.Precision.HIGHEST)
    slot_place = (jnp.sum(running_count * one_hot, axis=1) - 1.0).astype(jnp.int32)
    slot_index = flat_routes * capacity + slot_place
    slots = slot_index.reshape(rows_local, top_count).astype(jnp.float32)
    info = jnp.concatenate([slots.T, route_weight.T], axis=0)
    layer_out = routed_experts(
        info, normed, hidden1, expert_gate, expert_up, expert_down,
        shared_gate, shared_up, shared_down, capacity,
    )
    return layer_out.astype(jnp.bfloat16)


def solution(mesh):
    placed = (
        P("sp", "tp"),
        P("sp", "tp"),
        P("sp", "tp"),
        P(("sp", "tp"), None),
        P(),
        P(),
        P(),
        P(),
        P(("sp", "tp"), None),
        P(("sp", "tp"), None),
        P(("sp", "tp"), None, None),
        P(("sp", "tp"), None, None),
        P(("sp", "tp"), None, None),
        P(),
        P(),
        P(),
    )
    return jax.shard_map(
        body, mesh=mesh, in_specs=placed, out_specs=P(("sp", "tp"), None), check_vma=False
    )
```
